32 devices in a mesh: ep: 32 (over z, y, x, core).
Axes of the slice: x: 2, y: 2, z: 4, core: 2. Of those that a mesh axis runs over, the one named last changes fastest.
Arguments:
- tokens: bfloat16 [4096, 2048], P('ep'), may hold values from -6 to 6
- norm_gain: float32 [2048], replicated, may hold values from 0.1 to 1.9
- expert_ids: int32 [4096, 4], P('ep'), may hold values from 0 to 63, as said below
- gate_weights: float32 [4096, 4], P('ep'), may hold values from 0.1 to 0.6
- expert_gate: bfloat16 [64, 2048, 512], P('ep'), may hold values from -0.125 to 0.125
- expert_up: bfloat16 [64, 2048, 512], P('ep'), may hold values from -0.125 to 0.125
- expert_down: bfloat16 [64, 512, 2048], P('ep'), may hold values from -0.25 to 0.25
- shared_gate: bfloat16 [2048, 512], P('ep'), may hold values from -0.125 to 0.125
- shared_up: bfloat16 [2048, 512], P('ep'), may hold values from -0.125 to 0.125
- shared_down: bfloat16 [512, 2048], P(None, 'ep'), may hold values from -0.25 to 0.25
Outputs:
- mixed: bfloat16 [4096, 2048], P('ep')
The draws below stay inside these ranges and needn't reach their ends.
Inputs may be any that keep to these rules, and one draw needn't show every extreme that they name: `expert_ids`: expert e belongs to device e // 2; each row names 4 experts of 4 different devices; among the rows of one device at most 24 name experts of any one device, hence at most 24 any one expert; in every aligned block of 128 rows exactly 24 rows name one and the same expert.
All inputs are finite; a program needn't handle non-finite values.
Results may differ from the reference program's by a relative error of at most 0.0067.
Values may be sent and summed in bfloat16 or wider, within the bound.
A program may use at most 128 MiB of HBM per device.

```python
import jax
import jax.numpy as jnp
from jax import lax

D = 2048
DE = 512
DS = 512
TOP_K = 4
EXP_DEV = 2
TOK_DEV = 128
EXPERTS = 64
TOKENS = 4096


def route_block(block_key):
    holders = EXPERTS // EXP_DEV
    total = TOK_DEV * TOP_K
    mean_rows = total // holders
    extra = mean_rows // 2
    key_order, key_moved, key_bits, key_rows = jax.random.split(block_key, 4)
    order = jax.random.permutation(key_order, holders).astype(jnp.int32)
    moved = jax.random.randint(key_moved, (holders // 2,), 0, extra + 1).astype(jnp.int32)
    moved = moved.at[0].set(extra)
    counts = jnp.full((holders,), mean_rows, jnp.int32)
    counts = counts.at[order[0::2]].add(moved).at[order[1::2]].add(-moved)
    ends = jnp.cumsum(counts).astype(jnp.int32)
    slots = jnp.arange(total, dtype=jnp.int32)
    slot_dev = jnp.sum((ends[None, :] <= slots[:, None]).astype(jnp.int32), axis=1).astype(jnp.int32)
    bits = jax.random.randint(key_bits, (total,), 0, EXP_DEV).astype(jnp.int32)
    bits = jnp.where(slot_dev == order[0], 0, bits).astype(jnp.int32)
    expert = (slot_dev * EXP_DEV + bits).astype(jnp.int32)
    row_perm = jax.random.permutation(key_rows, TOK_DEV).astype(jnp.int32)
    row_of = row_perm[slots % TOK_DEV]
    column = (slots // TOK_DEV).astype(jnp.int32)
    table = jnp.zeros((TOK_DEV, TOP_K), jnp.int32).at[row_of, column].set(expert)
    return table


def draw_expert_ids(key, part):
    base = jax.random.fold_in(key, 7117)
    keys = jax.random.split(base, TOKENS // TOK_DEV)
    tables = jax.vmap(route_block)(keys)
    return tables.reshape(TOKENS, TOP_K).astype(jnp.int32)


def levels(key, extent, cuts, low, high):
    gain = 1.0
    for dim, blocks in cuts:
        steps = jax.random.uniform(jax.random.fold_in(jax.random.fold_in(key, 6), dim), (blocks,), jnp.float32, low / len(cuts), high / len(cuts))
        gain = gain * jnp.repeat(jnp.exp(steps), extent[dim] // blocks).reshape((-1,) + (1,) * (len(extent) - 1 - dim))
    return gain


def bell_draw(own_key, dims, scale, bound, shards=(), held_as=jnp.bfloat16):
    result = scale * jax.random.normal(own_key, dims, jnp.float32)
    if shards:
        result = result * levels(own_key, dims, shards, -0.22, 0.18)
    return jnp.clip(result, -bound, bound).astype(held_as)


def setup_inputs(seed: int = 0) -> dict:
    splits = jax.random.split(jax.random.key(seed), 11)
    return {
        "tokens": bell_draw(splits[0], (TOKENS, D), 1.0, 6.0, ((0, 32),)),
        "norm_gain": jnp.clip(1.0 + 0.18 * jax.random.normal(splits[1], (D,), jnp.float32), 0.1, 1.9),
        "expert_ids": draw_expert_ids(jax.random.fold_in(splits[10], 71), 0),
        "gate_weights": jnp.clip(0.1 + 0.5 * jax.random.uniform(splits[3], (TOKENS, TOP_K), jnp.float32) ** levels(splits[3], (TOKENS, TOP_K), ((0, 32),), -0.2, 0.2), 0.1, 0.6),
        "expert_gate": bell_draw(splits[4], (EXPERTS, D, DE), D ** -0.5, 0.125, ((0, 32),)),
        "expert_up": bell_draw(splits[5], (EXPERTS, D, DE), D ** -0.5, 0.125, ((0, 32),)),
        "expert_down": bell_draw(splits[6], (EXPERTS, DE, D), DE ** -0.5, 0.25, ((0, 32),)),
        "shared_gate": bell_draw(splits[7], (D, DS), D ** -0.5, 0.125, ((0, 32),)),
        "shared_up": bell_draw(splits[8], (D, DS), D ** -0.5, 0.125, ((0, 32),)),
        "shared_down": bell_draw(splits[9], (DS, D), DS ** -0.5, 0.25, ((1, 32),)),
    }


EPS = 1e-06

def normalize(tokens, norm_gain):
    values = tokens.astype(jnp.float32)
    scaled = values * lax.rsqrt(lax.optimization_barrier(jnp.mean(values * values, axis=-1, keepdims=True)) + EPS)
    return (scaled * norm_gain.astype(jnp.float32)).astype(jnp.bfloat16)

def swiglu(inputs, w_gate, w_up, w_down):
    gate_val = jnp.dot(inputs, w_gate, preferred_element_type=jnp.float32)
    up_val = jnp.dot(inputs, w_up, preferred_element_type=jnp.float32)
    hidden = (jax.nn.silu(gate_val) * up_val).astype(jnp.bfloat16)
    return jnp.dot(hidden, w_down, preferred_element_type=jnp.float32)

def reference(tokens, norm_gain, expert_ids, gate_weights, expert_gate, expert_up, expert_down, shared_gate, shared_up, shared_down):
    normed = normalize(tokens, norm_gain)
    count_tok = normed.shape[0]
    width = normed.shape[1]
    assign = count_tok * TOP_K
    flat_ids = expert_ids.reshape(assign).astype(jnp.int32)
    ordering = jnp.argsort(flat_ids, stable=True).astype(jnp.int32)
    sorted_ids = flat_ids[ordering]
    sorted_tok = (ordering // TOP_K).astype(jnp.int32)
    sorted_wts = gate_weights.reshape(assign)[ordering]
    counts = jnp.bincount(flat_ids, length=EXPERTS).astype(jnp.int32)
    block_rows = 256
    padded = ((counts + block_rows - 1) // block_rows * block_rows).astype(jnp.int32)
    pad_end = jnp.cumsum(padded).astype(jnp.int32)
    pad_start = pad_end - padded
    cnt_start = (jnp.cumsum(counts).astype(jnp.int32) - counts).astype(jnp.int32)
    dest = (pad_start[sorted_ids] + jnp.arange(assign, dtype=jnp.int32) - cnt_start[sorted_ids]).astype(jnp.int32)
    blocks = -(-(assign + EXPERTS * (block_rows - 1)) // block_rows)
    total_rows = blocks * block_rows
    row_tok = jnp.full((total_rows,), count_tok, jnp.int32).at[dest].set(sorted_tok)
    row_wts = jnp.zeros((total_rows,), jnp.float32).at[dest].set(sorted_wts)
    block_expert = jnp.minimum(jnp.searchsorted(pad_end, jnp.arange(blocks, dtype=jnp.int32) * block_rows, side='right'), EXPERTS - 1).astype(jnp.int32)
    padded_x = jnp.concatenate([normed, jnp.zeros((1, width), jnp.bfloat16)], axis=0)

    def step(accum, inputs_blk):
        tok_blk, wts_blk, expert = inputs_blk
        picked = padded_x[tok_blk]
        output = swiglu(picked, expert_gate[expert], expert_up[expert], expert_down[expert]).astype(jnp.bfloat16)
        accum = accum.at[tok_blk].add(output.astype(jnp.float32) * wts_blk[:, None])
        return (accum, None)
    routed, _ = lax.scan(step, jnp.zeros((count_tok + 1, width), jnp.float32), (row_tok.reshape(blocks, block_rows), row_wts.reshape(blocks, block_rows), block_expert))
    shared = swiglu(normed, shared_gate, shared_up, shared_down)
    return (routed[:count_tok] + shared).astype(jnp.bfloat16)
```

```python
import functools

import jax
import jax.numpy as jnp
from jax import lax
from jax.experimental import pallas as pl
from jax.experimental.pallas import tpu as pltpu
from jax.sharding import PartitionSpec as P

EPS = 1e-06
GROUPS = 4
MESH = pl.DeviceIdType.MESH
ORDER = ((0, 1, 2, 3), (1, 0, 2, 3), (2, 3, 1, 0), (3, 2, 1, 0))
BACK = ((1, 2, 3), (2, 3, 0), (1, 0, 3), (2, 1, 0))


def normalize(tokens, norm_gain):
    values = tokens.astype(jnp.float32)
    scaled = values * lax.rsqrt(jnp.mean(values * values, axis=-1, keepdims=True) + EPS)
    return (scaled * norm_gain).astype(jnp.bfloat16)


def pick(table, row, column):
    value = jnp.int32(table[0][column])
    for i in range(1, len(table)):
        value = jnp.where(row == i, jnp.int32(table[i][column]), value)
    return value


def moe_kernel(
    plane, rows_sent, chunk,
    x_ref, pack_ref, unpack_ref, label_ref, weight_ref, gate_hbm, up_hbm, down_hbm,
    out_ref,
    gate, up, down, held, packed, got, back, above, below, partial, total,
    w_sem, zsend, zrecv, dsend, drecv, rsend, rrecv, psend, arecv, brecv,
):
    me = lax.axis_index("ep")
    z, p = me // plane, me % plane
    has_low, has_high = z > 0, z < GROUPS - 1
    rows = packed.shape[1] * packed.shape[2]
    width = x_ref.shape[1]

    weights = [
        pltpu.make_async_copy(src, dst, w_sem.at[i])
        for i, (src, dst) in enumerate(((gate_hbm, gate), (up_hbm, up), (down_hbm, down)))
    ]
    for copy in weights:
        copy.start()

    back[...] = jnp.zeros_like(back)
    barrier = pltpu.get_barrier_semaphore()

    def greet(device):
        pl.semaphore_signal(barrier, inc=1, device_id=(device,), device_id_type=MESH)

    for i in range(1, plane):
        greet(z * plane + (p + i) % plane)

    @pl.when(has_low)
    def _():
        greet(me - plane)

    @pl.when(has_high)
    def _():
        greet(me + plane)

    pl.semaphore_wait(
        barrier, plane - 1 + has_low.astype(jnp.int32) + has_high.astype(jnp.int32)
    )

    def along(src, g, direction):
        return pltpu.make_async_remote_copy(
            src_ref=src, dst_ref=held.at[g],
            send_sem=zsend.at[direction, g], recv_sem=zrecv.at[g],
            device_id=(me + (plane if direction else -plane),), device_id_type=MESH,
        )

    @pl.when(has_low)
    def _():
        along(x_ref, z, 0).start()

    @pl.when(has_high)
    def _():
        along(x_ref, z, 1).start()

    held[z] = x_ref[...]

    def dispatch_copy(g, q, i):
        return pltpu.make_async_remote_copy(
            src_ref=packed.at[g, q, pl.ds(0, rows_sent)],
            dst_ref=got.at[g, p, pl.ds(0, rows_sent)],
            send_sem=dsend.at[g, i], recv_sem=drecv.at[g, i],
            device_id=(z * plane + q,), device_id_type=MESH,
        )

    def return_copy(g, q, i):
        return pltpu.make_async_remote_copy(
            src_ref=got.at[g, q, pl.ds(0, rows_sent)],
            dst_ref=back.at[g, p, pl.ds(0, rows_sent)],
            send_sem=rsend.at[g, i], recv_sem=rrecv.at[g, i],
            device_id=(z * plane + q,), device_id_type=MESH,
        )

    def dispatch(step):
        g = pick(ORDER, z, step)
        if step:
            along(held.at[g], g, 0).wait_recv()

            @pl.when(jnp.logical_and(g > z, has_low))
            def _():
                along(held.at[g], g, 0).start()

            @pl.when(jnp.logical_and(g < z, has_high))
            def _():
                along(held.at[g], g, 1).start()

        for c in range(0, width, chunk):
            columns = pl.ds(c, chunk)
            packed[g, :, :, columns] = (
                jnp.dot(pack_ref[g], held[g, :, columns], preferred_element_type=jnp.float32)
                .astype(jnp.bfloat16)
                .reshape(packed.shape[1], packed.shape[2], chunk)
            )
        for i in range(1, plane):
            dispatch_copy(g, (p + i) % plane, i).start()
        got[g, p] = packed[g, p]

    def compute(step):
        g = pick(ORDER, z, step)
        for i in range(1, plane):
            dispatch_copy(g, (p + i) % plane, i).wait_recv()
        x = got[g].reshape(rows, width)
        label = label_ref[g]
        hidden = []
        for e in range(gate.shape[0]):
            gate_val = jnp.dot(x, gate[e], preferred_element_type=jnp.float32)
            up_val = jnp.dot(x, up[e], preferred_element_type=jnp.float32)
            value = gate_val / (1.0 + jnp.exp(-gate_val)) * up_val
            hidden.append(jnp.where(label == e, value, 0.0).astype(jnp.bfloat16))
        for c in range(0, width, chunk):
            columns = pl.ds(c, chunk)
            value = jnp.zeros((rows, chunk), jnp.float32)
            for e in range(gate.shape[0]):
                value += jnp.dot(
                    hidden[e], down[e, :, columns], preferred_element_type=jnp.float32
                )
            got[g, :, :, columns] = (
                (value * weight_ref[g])
                .astype(jnp.bfloat16)
                .reshape(got.shape[1], got.shape[2], chunk)
            )
        for i in range(1, plane):
            return_copy(g, (p + i) % plane, i).start()
        back[g, p] = got[g, p]

    def partial_copy(g, upward):
        landing, sem = (below, brecv) if upward else (above, arecv)
        return pltpu.make_async_remote_copy(
            src_ref=partial.at[g], dst_ref=landing.at[g],
            send_sem=psend.at[g], recv_sem=sem.at[g],
            device_id=(me + (plane if upward else -plane),), device_id_type=MESH,
        )

    def combine(g):
        for i in range(1, plane):
            return_copy(g, (p + i) % plane, i).wait_recv()
        for c in range(0, width, chunk):
            columns = pl.ds(c, chunk)
            total[:, columns] = jnp.dot(
                unpack_ref[g],
                back[g, :, :, columns].reshape(rows, chunk),
                preferred_element_type=jnp.float32,
            )

        @pl.when(jnp.logical_and(g <= z, has_high))
        def _():
            partial_copy(g, False).wait_recv()
            total[...] += above[g].astype(jnp.float32)

        @pl.when(jnp.logical_and(g >= z, has_low))
        def _():
            partial_copy(g, True).wait_recv()
            total[...] += below[g].astype(jnp.float32)

    dispatch(0)
    dispatch(1)
    for copy in weights:
        copy.wait()
    compute(0)
    dispatch(2)
    compute(1)
    dispatch(3)
    compute(2)
    compute(3)
    for step in range(GROUPS - 1):
        g = pick(BACK, z, step)
        combine(g)
        partial[g] = total[...].astype(jnp.bfloat16)

        @pl.when(g > z)
        def _():
            partial_copy(g, True).start()

        @pl.when(g < z)
        def _():
            partial_copy(g, False).start()

    combine(z)
    out_ref[...] = total[...]

    for g in range(GROUPS):
        for i in range(1, plane):
            q = (p + i) % plane
            dispatch_copy(g, q, i).wait_send()
            return_copy(g, q, i).wait_send()

        @pl.when(jnp.logical_and(g >= z, has_low))
        def _():
            along(held.at[g], g, 0).wait_send()

        @pl.when(jnp.logical_and(g <= z, has_high))
        def _():
            along(held.at[g], g, 1).wait_send()

        @pl.when(g != z)
        def _():
            partial_copy(g, True).wait_send()


def routed_sum(normed, pack, unpack, label, weight, expert_gate, expert_up, expert_down, capacity):
    count_tok, width = normed.shape
    groups, rows, _ = pack.shape
    plane = lax.axis_size("ep") // groups
    padded = rows // plane
    bf16 = jnp.bfloat16
    rows_sent = -(-capacity // 8) * 8
    blocks = (groups, plane, padded, width)
    whole = (groups, count_tok, width)
    dma = pltpu.SemaphoreType.DMA
    vmem = pl.BlockSpec(memory_space=pltpu.VMEM)
    hbm = pl.BlockSpec(memory_space=pl.ANY)
    return pl.pallas_call(
        functools.partial(moe_kernel, plane, rows_sent, width // 4),
        out_shape=jax.ShapeDtypeStruct((count_tok, width), jnp.float32),
        in_specs=[vmem] * 5 + [hbm] * 3,
        out_specs=vmem,
        scratch_shapes=[
            pltpu.VMEM(expert_gate.shape, bf16),
            pltpu.VMEM(expert_up.shape, bf16),
            pltpu.VMEM(expert_down.shape, bf16),
            pltpu.VMEM(whole, bf16),
            pltpu.VMEM(blocks, bf16),
            pltpu.VMEM(blocks, bf16),
            pltpu.VMEM(blocks, bf16),
            pltpu.VMEM(whole, bf16),
            pltpu.VMEM(whole, bf16),
            pltpu.VMEM(whole, bf16),
            pltpu.VMEM((count_tok, width), jnp.float32),
            dma((3,)),
            dma((2, groups)),
            dma((groups,)),
            dma((groups, plane)),
            dma((groups, plane)),
            dma((groups, plane)),
            dma((groups, plane)),
            dma((groups,)),
            dma((groups,)),
            dma((groups,)),
        ],
        compiler_params=pltpu.CompilerParams(
            collective_id=0, has_side_effects=True, vmem_limit_bytes=60 * 1024 * 1024
        ),
    )(normed, pack, unpack, label, weight, expert_gate, expert_up, expert_down)


def per_device(
    tokens, norm_gain, expert_ids, gate_weights, expert_gate, expert_up, expert_down,
    shared_gate, shared_up, shared_down,
):
    f32, bf16 = jnp.float32, jnp.bfloat16
    normed = normalize(tokens, norm_gain)
    count_tok, top = expert_ids.shape
    local_experts = expert_gate.shape[0]
    devices = lax.axis_size("ep")
    plane = devices // GROUPS
    mean_rows = count_tok * top // devices
    capacity = mean_rows + mean_rows // 2
    padded = -(-capacity // 16) * 16
    me = lax.axis_index("ep")
    z, p = me // plane, me % plane

    small = jnp.concatenate([expert_ids.astype(f32), gate_weights], axis=1)
    small = lax.all_gather(small, "ep", axis=0)
    ids = small[:, :, :top].astype(jnp.int32)
    weights = small[:, :, top:]
    target = ids // local_experts
    slots = jnp.arange(padded, dtype=f32)
    earlier = jnp.tril(jnp.ones((count_tok, count_tok), bf16), -1)

    column = lax.dynamic_slice_in_dim(
        target.reshape(GROUPS, plane, count_tok, top), p, 1, axis=1
    )[:, 0]
    here = z * plane + jnp.arange(plane, dtype=jnp.int32)
    named = jnp.any(column[:, :, :, None] == here, axis=2)
    rank = jnp.einsum("ut,gtq->guq", earlier, named.astype(bf16), preferred_element_type=f32)
    rank = jnp.where(named, rank, -1.0)
    unpack = (rank[:, :, :, None] == slots).astype(bf16)
    unpack = unpack.reshape(GROUPS, count_tok, plane * padded)
    rank_t = rank.transpose(0, 2, 1)
    pack = (rank_t[:, :, None, :] == slots[:, None]).astype(bf16)
    pack = pack.reshape(GROUPS, plane * padded, count_tok)

    mine = target == me
    came = jnp.any(mine, axis=2)
    rank_in = jnp.einsum("ut,st->su", earlier, came.astype(bf16), preferred_element_type=f32)
    rank_in = jnp.where(came, rank_in, -1.0)
    slot_of = rank_in[:, None, :] == slots[:, None]
    which = jnp.sum(jnp.where(mine, ids % local_experts + 1, 0), axis=2)
    scale = jnp.sum(jnp.where(mine, weights, 0.0), axis=2)
    label = jnp.sum(jnp.where(slot_of, which[:, None, :], 0), axis=2) - 1
    weight = jnp.sum(jnp.where(slot_of, scale[:, None, :], 0.0), axis=2)
    label = label.reshape(GROUPS, plane * padded, 1)
    weight = weight.reshape(GROUPS, plane * padded, 1)

    routed = routed_sum(
        normed, pack, unpack, label, weight, expert_gate, expert_up, expert_down, capacity
    )

    shared_weights = jnp.concatenate([shared_gate, shared_up, shared_down.T], axis=1)
    shared_weights = lax.all_gather(shared_weights, "ep", axis=0, tiled=True)
    hidden = shared_gate.shape[1]
    gate_val = jnp.dot(normed, shared_weights[:, :hidden], preferred_element_type=f32)
    up_val = jnp.dot(normed, shared_weights[:, hidden : 2 * hidden], preferred_element_type=f32)
    shared_hidden = (jax.nn.silu(gate_val) * up_val).astype(bf16)
    shared = jnp.einsum(
        "th,dh->td", shared_hidden, shared_weights[:, 2 * hidden :], preferred_element_type=f32
    )
    return (routed + shared).astype(bf16)


def solution(mesh):
    return jax.shard_map(
        per_device,
        mesh=mesh,
        in_specs=(
            P("ep", None),
            P(),
            P("ep", None),
            P("ep", None),
            P("ep", None, None),
            P("ep", None, None),
            P("ep", None, None),
            P("ep", None),
            P("ep", None),
            P(None, "ep"),
        ),
        out_specs=P("ep", None),
        check_vma=False,
    )
```

```python
import functools

import jax
import jax.numpy as jnp
from jax import lax
from jax.experimental import pallas as pl
from jax.experimental.pallas import tpu as pltpu
from jax.sharding import PartitionSpec as P

EPS = 1e-06
GROUPS = 4
MESH = pl.DeviceIdType.MESH
ORDER = ((0, 1, 2, 3), (1, 0, 2, 3), (2, 3, 1, 0), (3, 2, 1, 0))
BACK = ((1, 2, 3), (2, 3, 0), (1, 0, 3), (2, 1, 0))


def normalize(tokens, norm_gain):
    values = tokens.astype(jnp.float32)
    scaled = values * lax.rsqrt(jnp.mean(values * values, axis=-1, keepdims=True) + EPS)
    return (scaled * norm_gain).astype(jnp.bfloat16)


def pick(table, row, column):
    value = jnp.int32(table[0][column])
    for i in range(1, len(table)):
        value = jnp.where(row == i, jnp.int32(table[i][column]), value)
    return value


def moe_kernel(
    plane, rows_sent, chunk,
    x_ref, pack_ref, unpack_ref, label_ref, weight_ref, slices_ref, gate_hbm, up_hbm, down_hbm,
    out_ref,
    gate, up, down, held, packed, got, back, above, below, partial, total, spread, shared,
    w_sem, zsend, zrecv, dsend, drecv, rsend, rrecv, psend, arecv, brecv,
    hzsend, hzrecv, hpsend, hprecv, hcsend, hcrecv,
):
    me = lax.axis_index("ep")
    z, p = me // plane, me % plane
    has_low, has_high = z > 0, z < GROUPS - 1
    rows = packed.shape[1] * packed.shape[2]
    part = shared.shape[1] // 3
    width = x_ref.shape[1]

    weights = [
        pltpu.make_async_copy(src, dst, w_sem.at[i])
        for i, (src, dst) in enumerate(((gate_hbm, gate), (up_hbm, up), (down_hbm, down)))
    ]
    for copy in weights:
        copy.start()

    back[...] = jnp.zeros_like(back)
    barrier = pltpu.get_barrier_semaphore()

    def greet(device):
        pl.semaphore_signal(barrier, inc=1, device_id=(device,), device_id_type=MESH)

    for i in range(1, plane):
        greet(z * plane + (p + i) % plane)

    for j in range(1, GROUPS):
        greet((z + j) % GROUPS * plane + p)
    pl.semaphore_wait(barrier, plane - 1 + GROUPS - 1)

    chips, chip, core = plane // 2, p // 2, p % 2

    def slice_copy(j):
        g = (z + j) % GROUPS
        return pltpu.make_async_remote_copy(
            src_ref=slices_ref.at[g], dst_ref=spread.at[core, chip, z],
            send_sem=hzsend.at[g], recv_sem=hzrecv.at[z],
            device_id=(g * plane + p,), device_id_type=MESH,
        )

    def slice_wait(j):
        g = (z + j) % GROUPS
        pltpu.make_async_remote_copy(
            src_ref=slices_ref.at[g], dst_ref=spread.at[core, chip, g],
            send_sem=hzsend.at[g], recv_sem=hzrecv.at[g],
            device_id=(g * plane + p,), device_id_type=MESH,
        ).wait_recv()

    def column_copy(i):
        return pltpu.make_async_remote_copy(
            src_ref=spread.at[core, chip], dst_ref=spread.at[core, chip],
            send_sem=hpsend.at[i], recv_sem=hprecv.at[i],
            device_id=(z * plane + (chip + i) % chips * 2 + core,), device_id_type=MESH,
        )

    def core_copy():
        return pltpu.make_async_remote_copy(
            src_ref=spread.at[core], dst_ref=spread.at[core],
            send_sem=hcsend.at[0], recv_sem=hcrecv.at[0],
            device_id=(me + 1 - 2 * core,), device_id_type=MESH,
        )

    for j in range(1, GROUPS):
        slice_copy(j).start()

    def along(src, g, direction):
        return pltpu.make_async_remote_copy(
            src_ref=src, dst_ref=held.at[g],
            send_sem=zsend.at[direction, g], recv_sem=zrecv.at[g],
            device_id=(me + (plane if direction else -plane),), device_id_type=MESH,
        )

    @pl.when(has_low)
    def _():
        along(x_ref, z, 0).start()

    @pl.when(has_high)
    def _():
        along(x_ref, z, 1).start()

    held[z] = x_ref[...]
    spread[core, chip, z] = slices_ref[z]

    def dispatch_copy(g, q, i):
        return pltpu.make_async_remote_copy(
            src_ref=packed.at[g, q, pl.ds(0, rows_sent)],
            dst_ref=got.at[g, p, pl.ds(0, rows_sent)],
            send_sem=dsend.at[g, i], recv_sem=drecv.at[g, i],
            device_id=(z * plane + q,), device_id_type=MESH,
        )

    def return_copy(g, q, i):
        return pltpu.make_async_remote_copy(
            src_ref=got.at[g, q, pl.ds(0, rows_sent)],
            dst_ref=back.at[g, p, pl.ds(0, rows_sent)],
            send_sem=rsend.at[g, i], recv_sem=rrecv.at[g, i],
            device_id=(z * plane + q,), device_id_type=MESH,
        )

    def dispatch(step):
        g = pick(ORDER, z, step)
        if step:
            along(held.at[g], g, 0).wait_recv()

            @pl.when(jnp.logical_and(g > z, has_low))
            def _():
                along(held.at[g], g, 0).start()

            @pl.when(jnp.logical_and(g < z, has_high))
            def _():
                along(held.at[g], g, 1).start()

        for c in range(0, width, chunk):
            columns = pl.ds(c, chunk)
            packed[g, :, :, columns] = (
                jnp.dot(pack_ref[g], held[g, :, columns], preferred_element_type=jnp.float32)
                .astype(jnp.bfloat16)
                .reshape(packed.shape[1], packed.shape[2], chunk)
            )
        for i in range(1, plane):
            dispatch_copy(g, (p + i) % plane, i).start()
        got[g, p] = packed[g, p]

    def compute(step):
        g = pick(ORDER, z, step)
        for i in range(1, plane):
            dispatch_copy(g, (p + i) % plane, i).wait_recv()
        x = got[g].reshape(rows, width)
        label = label_ref[g]
        hidden = []
        for e in range(gate.shape[0]):
            gate_val = jnp.dot(x, gate[e], preferred_element_type=jnp.float32)
            up_val = jnp.dot(x, up[e], preferred_element_type=jnp.float32)
            value = gate_val / (1.0 + jnp.exp(-gate_val)) * up_val
            hidden.append(jnp.where(label == e, value, 0.0).astype(jnp.bfloat16))
        for c in range(0, width, chunk):
            columns = pl.ds(c, chunk)
            value = jnp.zeros((rows, chunk), jnp.float32)
            for e in range(gate.shape[0]):
                value += jnp.dot(
                    hidden[e], down[e, :, columns], preferred_element_type=jnp.float32
                )
            got[g, :, :, columns] = (
                (value * weight_ref[g])
                .astype(jnp.bfloat16)
                .reshape(got.shape[1], got.shape[2], chunk)
            )
        for i in range(1, plane):
            return_copy(g, (p + i) % plane, i).start()
        back[g, p] = got[g, p]

    def partial_copy(g, upward):
        landing, sem = (below, brecv) if upward else (above, arecv)
        return pltpu.make_async_remote_copy(
            src_ref=partial.at[g], dst_ref=landing.at[g],
            send_sem=psend.at[g], recv_sem=sem.at[g],
            device_id=(me + (plane if upward else -plane),), device_id_type=MESH,
        )

    def combine(g):
        for i in range(1, plane):
            return_copy(g, (p + i) % plane, i).wait_recv()
        for c in range(0, width, chunk):
            columns = pl.ds(c, chunk)
            total[:, columns] = jnp.dot(
                unpack_ref[g],
                back[g, :, :, columns].reshape(rows, chunk),
                preferred_element_type=jnp.float32,
            )

        x = held[g]
        gate_val = jnp.dot(x, shared[:, :part], preferred_element_type=jnp.float32)
        up_val = jnp.dot(x, shared[:, part : 2 * part], preferred_element_type=jnp.float32)
        hidden = (gate_val / (1.0 + jnp.exp(-gate_val)) * up_val).astype(jnp.bfloat16)
        for c in range(0, width, chunk):
            total[:, c : c + chunk] += lax.dot_general(
                hidden, shared[c : c + chunk, 2 * part :], (((1,), (1,)), ((), ())),
                preferred_element_type=jnp.float32,
            )

        @pl.when(jnp.logical_and(g <= z, has_high))
        def _():
            partial_copy(g, False).wait_recv()
            total[...] += above[g].astype(jnp.float32)

        @pl.when(jnp.logical_and(g >= z, has_low))
        def _():
            partial_copy(g, True).wait_recv()
            total[...] += below[g].astype(jnp.float32)

    def pass_on(step):
        g = pick(BACK, z, step)
        combine(g)
        partial[g] = total[...].astype(jnp.bfloat16)

        @pl.when(g > z)
        def _():
            partial_copy(g, True).start()

        @pl.when(g < z)
        def _():
            partial_copy(g, False).start()

    dispatch(0)
    for j in range(1, GROUPS):
        slice_wait(j)
    for i in range(1, chips):
        column_copy(i).start()
    dispatch(1)
    for copy in weights:
        copy.wait()
    compute(0)
    dispatch(2)
    for i in range(1, chips):
        column_copy(i).wait_recv()
    core_copy().start()
    compute(1)
    dispatch(3)
    pltpu.make_async_remote_copy(
        src_ref=spread.at[core], dst_ref=spread.at[1 - core],
        send_sem=hcsend.at[0], recv_sem=hcrecv.at[0],
        device_id=(me + 1 - 2 * core,), device_id_type=MESH,
    ).wait_recv()
    piece = spread.shape[3]

    def lay(index, _):
        g, q = index // plane, index % plane
        start = pl.multiple_of(index * piece, piece)
        shared[pl.ds(start, piece), :] = spread[q % 2, q // 2, g]
        return 0

    lax.fori_loop(0, GROUPS * plane, lay, 0)
    compute(2)
    at_end = jnp.logical_not(jnp.logical_and(has_low, has_high))

    @pl.when(at_end)
    def _():
        pass_on(0)

    compute(3)

    @pl.when(jnp.logical_not(at_end))
    def _():
        pass_on(0)

    for step in range(1, GROUPS - 1):
        pass_on(step)
    combine(z)
    out_ref[...] = total[...].astype(out_ref.dtype)

    for j in range(1, GROUPS):
        slice_copy(j).wait_send()
    for i in range(1, chips):
        column_copy(i).wait_send()
    core_copy().wait_send()

    for g in range(GROUPS):
        for i in range(1, plane):
            q = (p + i) % plane
            dispatch_copy(g, q, i).wait_send()
            return_copy(g, q, i).wait_send()

        @pl.when(jnp.logical_and(g >= z, has_low))
        def _():
            along(held.at[g], g, 0).wait_send()

        @pl.when(jnp.logical_and(g <= z, has_high))
        def _():
            along(held.at[g], g, 1).wait_send()

        @pl.when(g != z)
        def _():
            partial_copy(g, True).wait_send()


def mixed_sum(
    normed, pack, unpack, label, weight, slices, expert_gate, expert_up, expert_down, capacity
):
    count_tok, width = normed.shape
    groups, rows, _ = pack.shape
    plane = lax.axis_size("ep") // groups
    padded = rows // plane
    bf16 = jnp.bfloat16
    rows_sent = -(-capacity // 8) * 8
    blocks = (groups, plane, padded, width)
    whole = (groups, count_tok, width)
    dma = pltpu.SemaphoreType.DMA
    vmem = pl.BlockSpec(memory_space=pltpu.VMEM)
    hbm = pl.BlockSpec(memory_space=pl.ANY)
    return pl.pallas_call(
        functools.partial(moe_kernel, plane, rows_sent, width // 4),
        out_shape=jax.ShapeDtypeStruct((count_tok, width), bf16),
        in_specs=[vmem] * 6 + [hbm] * 3,
        out_specs=vmem,
        scratch_shapes=[
            pltpu.VMEM(expert_gate.shape, bf16),
            pltpu.VMEM(expert_up.shape, bf16),
            pltpu.VMEM(expert_down.shape, bf16),
            pltpu.VMEM(whole, bf16),
            pltpu.VMEM(blocks, bf16),
            pltpu.VMEM(blocks, bf16),
            pltpu.VMEM(blocks, bf16),
            pltpu.VMEM(whole, bf16),
            pltpu.VMEM(whole, bf16),
            pltpu.VMEM(whole, bf16),
            pltpu.VMEM((count_tok, width), jnp.float32),
            pltpu.VMEM((2, plane // 2) + slices.shape, bf16),
            pltpu.VMEM((width, slices.shape[2]), bf16),
            dma((3,)),
            dma((2, groups)),
            dma((groups,)),
            dma((groups, plane)),
            dma((groups, plane)),
            dma((groups, plane)),
            dma((groups, plane)),
            dma((groups,)),
            dma((groups,)),
            dma((groups,)),
            dma((groups,)),
            dma((groups,)),
            dma((plane // 2,)),
            dma((plane // 2,)),
            dma((1,)),
            dma((1,)),
        ],
        compiler_params=pltpu.CompilerParams(
            collective_id=0, has_side_effects=True, vmem_limit_bytes=60 * 1024 * 1024
        ),
    )(normed, pack, unpack, label, weight, slices, expert_gate, expert_up, expert_down)


def spread_kernel(n, x_ref, out_ref, landed, send_sem, recv_sem):
    me = lax.axis_index("ep")
    barrier = pltpu.get_barrier_semaphore()
    for i in range(1, n):
        pl.semaphore_signal(barrier, inc=1, device_id=((me + i) % n,), device_id_type=MESH)
    pl.semaphore_wait(barrier, n - 1)

    def copy(i):
        return pltpu.make_async_remote_copy(
            src_ref=x_ref, dst_ref=landed.at[me],
            send_sem=send_sem.at[i], recv_sem=recv_sem.at[i],
            device_id=((me + i) % n,), device_id_type=MESH,
        )

    for i in range(1, n):
        copy(i).start()
    landed[me] = x_ref[...]
    for i in range(1, n):
        copy(i).wait_recv()
    out_ref[...] = landed[...]
    for i in range(1, n):
        copy(i).wait_send()


def gather_small(x):
    n = lax.axis_size("ep")
    vmem = pl.BlockSpec(memory_space=pltpu.VMEM)
    return pl.pallas_call(
        functools.partial(spread_kernel, n),
        out_shape=jax.ShapeDtypeStruct((n,) + x.shape, x.dtype),
        in_specs=[vmem],
        out_specs=vmem,
        scratch_shapes=[
            pltpu.VMEM((n,) + x.shape, x.dtype),
            pltpu.SemaphoreType.DMA((n,)),
            pltpu.SemaphoreType.DMA((n,)),
        ],
        compiler_params=pltpu.CompilerParams(collective_id=1, has_side_effects=True),
    )(x)


def per_device(
    tokens, norm_gain, expert_ids, gate_weights, expert_gate, expert_up, expert_down,
    shared_gate, shared_up, shared_down,
):
    f32, bf16 = jnp.float32, jnp.bfloat16
    normed = normalize(tokens, norm_gain)
    count_tok, top = expert_ids.shape
    local_experts = expert_gate.shape[0]
    devices = lax.axis_size("ep")
    plane = devices // GROUPS
    mean_rows = count_tok * top // devices
    capacity = mean_rows + mean_rows // 2
    padded = -(-capacity // 16) * 16
    me = lax.axis_index("ep")
    z, p = me // plane, me % plane

    small = jnp.concatenate([expert_ids.T.astype(f32), gate_weights.T], axis=0)
    small = gather_small(small)
    ids = small[:, :top].astype(jnp.int32)
    weights = small[:, top:]
    target = ids // local_experts
    slots = jnp.arange(padded, dtype=f32)
    earlier = jnp.tril(jnp.ones((count_tok, count_tok), bf16), -1)

    column = lax.dynamic_slice_in_dim(
        target.reshape(GROUPS, plane, top, count_tok), p, 1, axis=1
    )[:, 0]
    here = z * plane + jnp.arange(plane, dtype=jnp.int32)
    named = jnp.any(column[:, None] == here[:, None, None], axis=2)
    rank = jnp.einsum("ut,gqt->gqu", earlier, named.astype(bf16), preferred_element_type=f32)
    rank = jnp.where(named, rank, -1.0)
    pack = (rank[:, :, None, :] == slots[:, None]).astype(bf16)
    pack = pack.reshape(GROUPS, plane * padded, count_tok)
    unpack = (rank.transpose(0, 2, 1)[:, :, :, None] == slots).astype(bf16)
    unpack = unpack.reshape(GROUPS, count_tok, plane * padded)

    mine = target == me
    came = jnp.any(mine, axis=1)
    rank_in = jnp.einsum("ut,st->su", earlier, came.astype(bf16), preferred_element_type=f32)
    rank_in = jnp.where(came, rank_in, -1.0)
    slot_of = rank_in[:, None, :] == slots[:, None]
    which = jnp.sum(jnp.where(mine, ids % local_experts + 1, 0), axis=1)
    scale = jnp.sum(jnp.where(mine, weights, 0.0), axis=1)
    label = jnp.sum(jnp.where(slot_of, which[:, None, :], 0), axis=2) - 1
    weight = jnp.sum(jnp.where(slot_of, scale[:, None, :], 0.0), axis=2)
    label = label.reshape(GROUPS, plane * padded, 1)
    weight = weight.reshape(GROUPS, plane * padded, 1)

    depth = shared_gate.shape[0]
    slices = jnp.concatenate(
        [w.reshape(depth, GROUPS, -1) for w in (shared_gate, shared_up, shared_down.T)], axis=2
    ).transpose(1, 0, 2)
    return mixed_sum(
        normed, pack, unpack, label, weight, slices, expert_gate, expert_up, expert_down, capacity
    )


def solution(mesh):
    return jax.shard_map(
        per_device,
        mesh=mesh,
        in_specs=(
            P("ep", None),
            P(),
            P("ep", None),
            P("ep", None),
            P("ep", None, None),
            P("ep", None, None),
            P("ep", None, None),
            P("ep", None),
            P("ep", None),
            P(None, "ep"),
        ),
        out_specs=P("ep", None),
        check_vma=False,
    )
```
